32 devices in a mesh: sp: 8 (over z, y), tp: 4 (over x, core).
Axes of the slice: x: 2, y: 2, z: 4, core: 2. Of those that a mesh axis runs over, the one named last changes fastest.
Arguments:
- prompt: bfloat16 [4, 1536, 4096], P(None, 'sp'), may hold values from -6 to 6
- forget_weight: bfloat16 [4096, 2048], P(None, 'tp'), may hold values from -0.09375 to 0.09375
- value_weight: bfloat16 [4096, 2048], P(None, 'tp'), may hold values from -1.5 to 1.5
- lower_bound: float32 [2048], P('tp'), may hold values from 0.9 to 0.9996745
- extra_decay: float32 [4, 1536, 2048], P(None, 'sp', 'tp'), may hold values from -1.4045573 to 0
- new_token: bfloat16 [4, 4096], P(None, 'tp'), may hold values from -6 to 6
- new_query: bfloat16 [4, 2048], P(None, 'tp'), may hold values from -6 to 6
- read_gain: float32 [128], replicated, may hold values from 0.1 to 1.9
Outputs:
- state_cache: bfloat16 [128, 16, 4, 128], P('sp', 'tp')
- first_read: bfloat16 [4, 2048], P(None, 'tp')
The draws below stay inside these ranges and needn't reach their ends.
All inputs are finite; a program needn't handle non-finite values.
Results may differ from the reference program's by a relative error of at most 0.0019.
The reference program's roundings to bfloat16 on the way (of `forget_pre`, `values` and `weighted`) count: a program that leaves them out, or rounds other values in their place, can miss the bound.
Values may be sent and summed in bfloat16 or wider, within the bound.
A program may use at most 64 MiB of HBM per device.

```python
import math
import jax
import jax.numpy as jnp
from jax import lax

D = 4096
H = 16
HD = 128
PROMPT_COUNT = 4
SPAN = 192
W = 2048
SEQLEN = 1536


def draw_prompt(key, part):
    base_key = jax.random.fold_in(key, 5)
    drawn = jnp.clip(jax.random.normal(base_key, (PROMPT_COUNT, SEQLEN, D), jnp.float32), -6.0, 6.0)
    positions = jnp.arange(SEQLEN, dtype=jnp.int32)
    quiet = jnp.where(positions >= SEQLEN - 3 * SPAN, 0.03, 1.0).astype(jnp.float32)
    return (drawn * quiet[None, :, None]).astype(jnp.bfloat16)


def draw_lower_bound(key, part):
    head_key, slow_key, fast_key = jax.random.split(jax.random.fold_in(key, 11), 3)
    share = 0.5
    fast_heads = jax.random.bernoulli(head_key, share, (H,))
    fast_cols = jnp.repeat(fast_heads, HD)
    slow_value = 1.0 - jax.random.uniform(slow_key, (H * HD,), jnp.float32, 0.5, 1.5) / SEQLEN
    fast_value = jax.random.uniform(fast_key, (H * HD,), jnp.float32, 0.965, 0.98)
    return jnp.where(fast_cols, fast_value, slow_value).astype(jnp.float32)


def draw_extra_decay(key, part):
    decay_rate_key, jitter_random_key, location_random_key, spike_random_key, channel_random_key, mixing_random_key = jax.random.split(jax.random.fold_in(key, 23), 6)
    lower_rate, upper_rate = (0.25, 1.0)
    block_count = SEQLEN // SPAN
    block_rate = jnp.exp(jax.random.uniform(decay_rate_key, (PROMPT_COUNT, block_count, 1, 1), jnp.float32, math.log(lower_rate), math.log(upper_rate)))
    channel_factor = jnp.exp(jax.random.uniform(channel_random_key, (PROMPT_COUNT, 1, 1, W), jnp.float32, -1.0, 1.0))
    block_channel = jnp.exp(jax.random.uniform(mixing_random_key, (PROMPT_COUNT, block_count, 1, W), jnp.float32, -0.5, 0.5))
    roughness = jax.random.uniform(jitter_random_key, (PROMPT_COUNT, block_count, SPAN, W), jnp.float32, 0.5, 1.5)
    chosen_locations = jax.random.randint(location_random_key, (PROMPT_COUNT, 2), 0, SEQLEN)
    spike_length = jax.random.uniform(spike_random_key, (PROMPT_COUNT, 2), jnp.float32, 0.22, 0.69)
    token_positions = jnp.arange(SEQLEN, dtype=jnp.int32)
    spike_events = jnp.sum((token_positions[None, None, :] == chosen_locations[:, :, None]).astype(jnp.float32) * spike_length[:, :, None], axis=1)
    steady_baseline = (block_rate * channel_factor * block_channel * roughness).reshape(PROMPT_COUNT, SEQLEN, W) / SEQLEN
    return (-steady_baseline - spike_events[:, :, None]).astype(jnp.float32)


def block_scale(stream_key, dims, cuts, low, top_value):
    gain, own = 1.0, jax.random.fold_in(stream_key, 6)
    for axis_at, parts in cuts:
        draws = jnp.exp(jax.random.uniform(jax.random.fold_in(own, axis_at), (parts,), jnp.float32, low / len(cuts), top_value / len(cuts)))
        gain = gain * jnp.repeat(draws, dims[axis_at] // parts).reshape([-1 if axis == axis_at else 1 for axis in range(len(dims))])
    return gain


def centred(rng, dims, width, bound, pieces=(), held_as=jnp.bfloat16):
    values = jax.random.normal(rng, dims, jnp.float32) * width
    if len(pieces) > 0:
        values = block_scale(rng, dims, pieces, -0.22, 0.18) * values
    return jnp.clip(values, min=-bound, max=bound).astype(held_as)


def setup_inputs(seed: int = 0) -> dict:
    splits = jax.random.split(jax.random.key(seed), 9)
    return {
        "prompt": draw_prompt(jax.random.fold_in(splits[8], 71), 0),
        "forget_weight": centred(splits[1], (D, W), D ** -0.5, 0.09375, ((1, 4),)),
        "value_weight": centred(splits[2], (D, W), 0.25, 1.5, ((1, 4),)),
        "lower_bound": draw_lower_bound(jax.random.fold_in(splits[8], 71), 0),
        "extra_decay": draw_extra_decay(jax.random.fold_in(splits[8], 71), 0),
        "new_token": centred(splits[5], (PROMPT_COUNT, D), 1.0, 6.0, ((1, 4),)),
        "new_query": centred(splits[6], (PROMPT_COUNT, W), 1.0, 6.0, ((1, 4),)),
        "read_gain": jnp.clip(1.0 + 0.18 * jax.random.normal(splits[7], (HD,), jnp.float32), 0.1, 1.9),
    }


def reference(prompt, forget_weight, value_weight, lower_bound, extra_decay, new_token, new_query, read_gain):
    log_lower = jnp.log(lower_bound)
    log_upper = jnp.log1p(-lower_bound)
    opening = 1.0 - lower_bound
    head_count = W // HD
    block_count = SEQLEN // SPAN

    def one_sequence(seq_pair):
        tokens, extra_part = seq_pair
        forget_pre = lax.optimization_barrier(jnp.dot(tokens, forget_weight, preferred_element_type=jnp.float32).astype(jnp.bfloat16)).astype(jnp.float32)
        values = lax.optimization_barrier(jnp.dot(tokens, value_weight, preferred_element_type=jnp.float32).astype(jnp.bfloat16)).astype(jnp.float32)
        log_forget = jnp.logaddexp(log_lower, log_upper + jax.nn.log_sigmoid(forget_pre)) + extra_part
        key_rows = opening * jax.nn.sigmoid(-forget_pre)
        running = jnp.cumsum(log_forget.reshape(block_count, SPAN, W), axis=1)
        totals = running[:, -1]
        weighted = key_rows.reshape(block_count, SPAN, W) * jnp.exp(totals[:, None] - running)
        weighted = lax.optimization_barrier(weighted.astype(jnp.bfloat16)).astype(jnp.float32)
        weighted = weighted.reshape(block_count, SPAN, head_count, HD)
        value_rows = values.reshape(block_count, SPAN, head_count, HD)
        block_state = jnp.einsum('nthd,nthe->nhde', weighted, value_rows, precision=lax.Precision.HIGHEST)
        later_sum = jnp.cumsum(totals[::-1], axis=0)[::-1] - totals
        end_scale = jnp.exp(later_sum).reshape(block_count, head_count, HD)
        return lax.optimization_barrier(jnp.sum(end_scale[..., None] * block_state, axis=0))
    final_state = lax.map(one_sequence, (prompt, extra_decay))
    state_cache = final_state.transpose(2, 1, 0, 3).astype(jnp.bfloat16)
    new_forget = lax.optimization_barrier(jnp.dot(new_token, forget_weight, preferred_element_type=jnp.float32).astype(jnp.bfloat16)).astype(jnp.float32)
    new_value = lax.optimization_barrier(jnp.dot(new_token, value_weight, preferred_element_type=jnp.float32).astype(jnp.bfloat16)).astype(jnp.float32)
    new_log = jnp.logaddexp(log_lower, log_upper + jax.nn.log_sigmoid(new_forget))
    new_key = opening * jax.nn.sigmoid(-new_forget)
    query_act = jax.nn.silu(new_query.astype(jnp.float32)).reshape(PROMPT_COUNT, head_count, HD)
    updated = jnp.exp(new_log).reshape(PROMPT_COUNT, head_count, HD)[..., None] * final_state
    updated = updated + new_key.reshape(PROMPT_COUNT, head_count, HD)[..., None] * new_value.reshape(PROMPT_COUNT, head_count, 1, HD)
    raw_read = lax.optimization_barrier(jnp.sum(query_act[..., None] * updated, axis=2))
    normed = raw_read * lax.rsqrt(lax.optimization_barrier(jnp.mean(raw_read * raw_read, axis=-1, keepdims=True)) + 1e-06) * read_gain
    first_read = normed.reshape(PROMPT_COUNT, W).astype(jnp.bfloat16)
    return (state_cache, first_read)
```

```python
import functools

import jax
import jax.numpy as jnp
from jax import lax
from jax.experimental import pallas as pl
from jax.experimental.pallas import tpu as pltpu
from jax.sharding import PartitionSpec as P

HD = 128
PAD = 16
CHUNKS = 4
MESH = pl.DeviceIdType.MESH
F32 = jnp.float32
BF16 = jnp.bfloat16


def near_size(count):
    near = 1
    while near * near * 4 <= count:
        near *= 2
    return near


def kernel(
    n, m, near,
    prompt, forget_w, value_w, lower, extra, token, query, gain,
    state_out, read_out,
    xs, ws, ex, acc, toks, bs, ry, pz, rz, tb, rp, lcol, qk, kv,
    x_sem, w_sem, e_sem, tok_send, tok_recv, t_send, t_recv, y_send, y_recv,
    z_send, z_recv, r_send, r_recv,
):
    far = n // near
    seqs, span, depth = prompt.shape
    rows = seqs * span
    heads = forget_w.shape[1] // HD
    share = HD // n
    kc = depth // CHUNKS
    tk = token.shape[1]
    me, mt = lax.axis_index("sp"), lax.axis_index("tp")
    my_far, my_near = me // near, me % near

    x_copies, w_copies = [], {}
    for c in range(CHUNKS):
        ks = pl.ds(c * kc, kc)
        part = []
        for s in range(seqs):
            cp = pltpu.make_async_copy(
                prompt.at[s, :, ks], xs.at[pl.ds(s * span, span), ks], x_sem.at[c, s]
            )
            cp.start()
            part.append(cp)
        x_copies.append(part)
        for i, w in enumerate((forget_w, value_w)):
            cp = pltpu.make_async_copy(
                w.at[ks, pl.ds(0, HD)], ws.at[0, ks, pl.ds(i * HD, HD)], w_sem.at[0, c, i]
            )
            cp.start()
            w_copies[0, c, i] = cp
    e_copy = pltpu.make_async_copy(extra, ex, e_sem)
    e_copy.start()
    for h in range(1, heads):
        for c in range(CHUNKS):
            ks = pl.ds(c * kc, kc)
            for i, w in enumerate((forget_w, value_w)):
                cp = pltpu.make_async_copy(
                    w.at[ks, pl.ds(h * HD, HD)],
                    ws.at[h, ks, pl.ds(i * HD, HD)],
                    w_sem.at[h, c, i],
                )
                cp.start()
                w_copies[h, c, i] = cp

    barrier = pltpu.get_barrier_semaphore()
    for k in range(1, m):
        pl.semaphore_signal(
            barrier, inc=1, device_id={"tp": lax.rem(mt + k, m)}, device_id_type=MESH
        )
    for k in range(1, n):
        pl.semaphore_signal(
            barrier, inc=1, device_id={"sp": lax.rem(me + k, n)}, device_id_type=MESH
        )
    pl.semaphore_wait(barrier, n + m - 2)

    sends = []

    def send(src, dst, s_sem, r_sem, target):
        cp = pltpu.make_async_remote_copy(
            src_ref=src, dst_ref=dst, send_sem=s_sem, recv_sem=r_sem,
            device_id=target, device_id_type=MESH,
        )
        cp.start()
        sends.append(cp)
        return cp

    tok_copies = [
        send(token, toks.at[mt], tok_send.at[k], tok_recv.at[k], {"tp": lax.rem(mt + k, m)})
        for k in range(1, m)
    ]
    toks[mt] = token[...]

    def lanes(ref, h):
        return ref[pl.ds(h * HD, HD)].reshape(1, HD)

    def matmul(h):
        tall = rows if h == 0 else rows + PAD
        for c in range(CHUNKS):
            if h == 0:
                for cp in x_copies[c]:
                    cp.wait()
            for i in range(2):
                w_copies[h, c, i].wait()
            ks = pl.ds(c * kc, kc)
            part = jnp.dot(xs[pl.ds(0, tall), ks], ws[h, ks, :], preferred_element_type=F32)
            if c == 0:
                acc[h % 2, pl.ds(0, tall), :] = part
            else:
                acc[h % 2, pl.ds(0, tall), :] += part

    t_copies, y_copies, z_copies = {}, {}, {}

    def gate(h):
        opening = 1.0 - lanes(lower, h)
        at = lax.broadcasted_iota(jnp.int32, (span, HD), 0)

        def later(x, k):
            if k % 8 == 0:
                return jnp.concatenate([x[k:], jnp.ones((k, HD), F32)], axis=0)
            return jnp.where(at < span - k, pltpu.roll(x, span - k, 0), 1.0)

        for s in range(seqs):
            block = pl.ds(s * span, span)
            pre = acc[h % 2, block, pl.ds(0, HD)].astype(BF16).astype(F32)
            values = acc[h % 2, block, pl.ds(HD, HD)].astype(BF16)
            key = opening / (1.0 + jnp.exp(pre))
            keep = (1.0 - key) * jnp.exp(ex[s, :, pl.ds(h * HD, HD)])
            after = later(keep, 1)
            k = 1
            while k < span:
                after = after * later(after, k)
                k *= 2
            weighted = (key * after).astype(BF16)
            tb[h, me, pl.ds(s, 1), :] = after[0:1] * keep[0:1]
            state = lax.dot_general(
                weighted, values, (((0,), (0,)), ((), ())), preferred_element_type=F32
            )
            for f in range(far):
                for y in range(near):
                    lo = (f * near + y) * share
                    bs[h, y, f, s] = state[lo : lo + share]
        t_copies[h] = [
            send(tb.at[h, me], tb.at[h, me], t_send.at[h, k], t_recv.at[h, k],
                 {"sp": lax.rem(me + k, n)})
            for k in range(1, n)
        ]
        y_copies[h] = []
        for k in range(1, near):
            y = lax.rem(my_near + k, near)
            y_copies[h].append(
                send(bs.at[h, y], ry.at[h, k - 1], y_send.at[h, k - 1], y_recv.at[h, k - 1],
                     {"sp": my_far * near + y})
            )

    def scale_after(h, block):
        total = jnp.ones((seqs, HD), F32)
        for b in range(n):
            total = total * jnp.where(b > block, tb[h, b], 1.0)
        return total

    def combine(h):
        for cp in t_copies[h]:
            cp.wait_recv()
        sources = [lax.rem(my_near + near - k, near) for k in range(near)]
        scales = [scale_after(h, my_far * near + y) for y in sources]
        fill = HD - near * seqs
        cols = jnp.concatenate(scales + [jnp.zeros((fill, HD), F32)], axis=0).T
        for f in range(far):
            for y in range(near):
                lo = (f * near + y) * share
                lcol[h, y, f] = cols[lo : lo + share]
        for cp in y_copies[h]:
            cp.wait_recv()
        for f in range(far):
            col = lcol[h, my_near, f]
            for s in range(seqs):
                total = bs[h, my_near, f, s] * col[:, s : s + 1]
                for k in range(1, near):
                    j = k * seqs + s
                    total += ry[h, k - 1, f, s] * col[:, j : j + 1]
                pz[h, f, s] = total
        z_copies[h] = []
        for k in range(1, far):
            f = lax.rem(my_far + k, far)
            z_copies[h].append(
                send(pz.at[h, f], rz.at[h, k - 1], z_send.at[h, k - 1], z_recv.at[h, k - 1],
                     {"sp": f * near + my_near})
            )

    def finish(h):
        for cp in z_copies[h]:
            cp.wait_recv()
        for s in range(seqs):
            total = pz[h, my_far, s]
            for k in range(1, far):
                total += rz[h, k - 1, s]
            state_out[h, s] = total.astype(BF16)

    def token_terms(h, block):
        new_pre = block[0:seqs, 0:HD].astype(BF16).astype(F32)
        new_value = block[0:seqs, HD : 2 * HD].astype(BF16).astype(F32)
        new_key = (1.0 - lanes(lower, h)) / (1.0 + jnp.exp(new_pre))
        q = query[:, pl.ds(h * HD, HD)].astype(F32)
        q = q / (1.0 + jnp.exp(-q))
        qk[h] = q * (1.0 - new_key)
        kv[h] = jnp.sum(q * new_key, axis=1, keepdims=True) * new_value

    def read_part(h):
        row = qk[h] * scale_after(h, me)
        col = jnp.concatenate([row, jnp.zeros((HD - seqs, HD), F32)], axis=0).T
        for s in range(seqs):
            total = jnp.zeros((share, HD), F32)
            for f in range(far):
                for y in range(near):
                    lo = (f * near + y) * share
                    total += bs[h, y, f, s] * col[lo : lo + share, s : s + 1]
            rp[me, h, pl.ds(s, 1), :] = jnp.sum(total, axis=0, keepdims=True)

    e_waited = False
    for h in range(heads):
        if h == 1:
            for cp in tok_copies:
                cp.wait_recv()
            xs[pl.ds(rows, PAD), :] = jnp.zeros((PAD, depth), BF16)
            for c in range(m):
                xs[pl.ds(rows, seqs), pl.ds(c * tk, tk)] = toks[c]
        matmul(h)
        if not e_waited:
            e_copy.wait()
            e_waited = True
        gate(h)
        if h >= 1:
            token_terms(h, acc[h % 2, pl.ds(rows, PAD), :])
            combine(h - 1)
        if h >= 2:
            finish(h - 2)
    first = jnp.dot(xs[pl.ds(rows, PAD), :], ws[0], preferred_element_type=F32)
    token_terms(0, first)
    for h in range(heads - 1):
        read_part(h)
    combine(heads - 1)
    read_part(heads - 1)
    r_copies = [
        send(rp.at[me], rp.at[me], r_send.at[k], r_recv.at[k], {"sp": lax.rem(me + k, n)})
        for k in range(1, n)
    ]
    if heads > 1:
        finish(heads - 2)
    for cp in r_copies:
        cp.wait_recv()
    for h in range(heads):
        raw = kv[h]
        for b in range(n):
            raw = raw + rp[b, h]
        mean = jnp.mean(raw * raw, axis=1, keepdims=True)
        normed = raw * lax.rsqrt(mean + 1e-6) * lanes(gain, 0)
        read_out[:, pl.ds(h * HD, HD)] = normed.astype(BF16)
    finish(heads - 1)
    for cp in sends:
        cp.wait_send()


def local(n, m, prompt, forget_w, value_w, lower, extra, token, query, gain):
    seqs, span, depth = prompt.shape
    rows = seqs * span
    width = forget_w.shape[1]
    heads = width // HD
    share = HD // n
    near = near_size(n)
    far = n // near
    vmem = pl.BlockSpec(memory_space=pltpu.VMEM)
    hbm = pl.BlockSpec(memory_space=pl.ANY)
    dma = pltpu.SemaphoreType.DMA
    state, read = pl.pallas_call(
        functools.partial(kernel, n, m, near),
        out_shape=(
            jax.ShapeDtypeStruct((heads, seqs, share, HD), BF16),
            jax.ShapeDtypeStruct((seqs, width), BF16),
        ),
        in_specs=[hbm, hbm, hbm, vmem, hbm, vmem, vmem, vmem],
        out_specs=(vmem, vmem),
        scratch_shapes=[
            pltpu.VMEM((rows + PAD, depth), BF16),
            pltpu.VMEM((heads, depth, 2 * HD), BF16),
            pltpu.VMEM((seqs, span, width), F32),
            pltpu.VMEM((2, rows + PAD, 2 * HD), F32),
            pltpu.VMEM((m, seqs, token.shape[1]), BF16),
            pltpu.VMEM((heads, near, far, seqs, share, HD), F32),
            pltpu.VMEM((heads, near - 1, far, seqs, share, HD), F32),
            pltpu.VMEM((heads, far, seqs, share, HD), F32),
            pltpu.VMEM((heads, far - 1, seqs, share, HD), F32),
            pltpu.VMEM((heads, n, seqs, HD), F32),
            pltpu.VMEM((n, heads, seqs, HD), F32),
            pltpu.VMEM((heads, near, far, share, HD), F32),
            pltpu.VMEM((heads, seqs, HD), F32),
            pltpu.VMEM((heads, seqs, HD), F32),
            dma((CHUNKS, seqs)),
            dma((heads, CHUNKS, 2)),
            dma,
            dma((m,)),
            dma((m,)),
            dma((heads, n)),
            dma((heads, n)),
            dma((heads, near - 1)),
            dma((heads, near - 1)),
            dma((heads, far - 1)),
            dma((heads, far - 1)),
            dma((n,)),
            dma((n,)),
        ],
        compiler_params=pltpu.CompilerParams(collective_id=0, has_side_effects=True),
    )(prompt, forget_w, value_w, lower, extra, token, query, gain)
    return state.transpose(2, 0, 1, 3), read


def solution(mesh):
    return jax.shard_map(
        functools.partial(local, mesh.shape["sp"], mesh.shape["tp"]),
        mesh=mesh,
        in_specs=(
            P(None, "sp", None),
            P(None, "tp"),
            P(None, "tp"),
            P("tp"),
            P(None, "sp", "tp"),
            P(None, "tp"),
            P(None, "tp"),
            P(),
        ),
        out_specs=(P("sp", "tp", None, None), P(None, "tp")),
        check_vma=False,
    )
```

```python
import functools

import jax
import jax.numpy as jnp
from jax import lax
from jax.experimental import pallas as pl
from jax.experimental.pallas import tpu as pltpu
from jax.sharding import PartitionSpec as P

HD = 128
PAD = 16
CHUNKS = 4
GROUP = 2
MESH = pl.DeviceIdType.MESH
F32 = jnp.float32
BF16 = jnp.bfloat16


def near_size(count):
    near = 1
    while near * near * 4 <= count:
        near *= 2
    return near


def kernel(
    n, m, near,
    prompt, forget_w, value_w, lower, extra, token, query, gain,
    state_out, read_out,
    xs, ws, ex, acc, toks, bs, ry, pz, rz, tb, rp, lcol, qk, kv,
    x_sem, w_sem, e_sem, tok_send, tok_recv, t_send, t_recv, y_send, y_recv,
    z_send, z_recv, r_send, r_recv,
):
    far = n // near
    seqs, span, depth = prompt.shape
    rows = seqs * span
    heads = forget_w.shape[1] // HD
    groups, wide = heads // GROUP, GROUP * HD
    share = HD // n
    kc = depth // CHUNKS
    tk = token.shape[1]
    me, mt = lax.axis_index("sp"), lax.axis_index("tp")
    my_far, my_near = me // near, me % near

    x_copies, w_copies = [], {}
    for c in range(CHUNKS):
        ks = pl.ds(c * kc, kc)
        part = []
        for s in range(seqs):
            cp = pltpu.make_async_copy(
                prompt.at[s, :, ks], xs.at[pl.ds(s * span, span), ks], x_sem.at[c, s]
            )
            cp.start()
            part.append(cp)
        x_copies.append(part)
        for i, w in enumerate((forget_w, value_w)):
            cp = pltpu.make_async_copy(
                w.at[ks, pl.ds(0, wide)], ws.at[0, ks, pl.ds(i * wide, wide)], w_sem.at[0, c, i]
            )
            cp.start()
            w_copies[0, c, i] = cp
    e_copy = pltpu.make_async_copy(extra, ex, e_sem)
    e_copy.start()
    for g in range(1, groups):
        for c in range(CHUNKS):
            ks = pl.ds(c * kc, kc)
            for i, w in enumerate((forget_w, value_w)):
                cp = pltpu.make_async_copy(
                    w.at[ks, pl.ds(g * wide, wide)],
                    ws.at[g, ks, pl.ds(i * wide, wide)],
                    w_sem.at[g, c, i],
                )
                cp.start()
                w_copies[g, c, i] = cp

    barrier = pltpu.get_barrier_semaphore()
    for k in range(1, m):
        pl.semaphore_signal(
            barrier, inc=1, device_id={"tp": lax.rem(mt + k, m)}, device_id_type=MESH
        )
    for k in range(1, n):
        pl.semaphore_signal(
            barrier, inc=1, device_id={"sp": lax.rem(me + k, n)}, device_id_type=MESH
        )
    pl.semaphore_wait(barrier, n + m - 2)

    sends = []

    def send(src, dst, s_sem, r_sem, target):
        cp = pltpu.make_async_remote_copy(
            src_ref=src, dst_ref=dst, send_sem=s_sem, recv_sem=r_sem,
            device_id=target, device_id_type=MESH,
        )
        cp.start()
        sends.append(cp)
        return cp

    tok_copies = [
        send(token, toks.at[mt], tok_send.at[k], tok_recv.at[k], {"tp": lax.rem(mt + k, m)})
        for k in range(1, m)
    ]
    toks[mt] = token[...]

    def lanes(ref, h):
        return ref[pl.ds(h * HD, HD)].reshape(1, HD)

    def matmul(g):
        tall = rows if g == 0 else rows + PAD
        for c in range(CHUNKS):
            if g == 0:
                for cp in x_copies[c]:
                    cp.wait()
            for i in range(2):
                w_copies[g, c, i].wait()
            ks = pl.ds(c * kc, kc)
            part = jnp.dot(xs[pl.ds(0, tall), ks], ws[g, ks, :], preferred_element_type=F32)
            if c == 0:
                acc[g % 2, pl.ds(0, tall), :] = part
            else:
                acc[g % 2, pl.ds(0, tall), :] += part

    t_copies, y_copies, z_copies = {}, {}, {}

    def gate(h):
        g, i = h // GROUP, h % GROUP
        opening = 1.0 - lanes(lower, h)
        at = lax.broadcasted_iota(jnp.int32, (span, HD), 0)

        def later(x, k):
            if k % 8 == 0:
                return jnp.concatenate([x[k:], jnp.ones((k, HD), F32)], axis=0)
            return jnp.where(at < span - k, pltpu.roll(x, span - k, 0), 1.0)

        for s in range(seqs):
            block = pl.ds(s * span, span)
            pre = acc[g % 2, block, pl.ds(i * HD, HD)].astype(BF16).astype(F32)
            values = acc[g % 2, block, pl.ds(wide + i * HD, HD)].astype(BF16)
            key = opening / (1.0 + jnp.exp(pre))
            keep = (1.0 - key) * jnp.exp(ex[s, :, pl.ds(h * HD, HD)])
            after = later(keep, 1)
            k = 1
            while k < span:
                after = after * later(after, k)
                k *= 2
            weighted = (key * after).astype(BF16)
            tb[g, me, i, pl.ds(s, 1), :] = after[0:1] * keep[0:1]
            state = lax.dot_general(
                weighted, values, (((0,), (0,)), ((), ())), preferred_element_type=F32
            )
            for f in range(far):
                for y in range(near):
                    lo = (f * near + y) * share
                    bs[h, y, f, s] = state[lo : lo + share]

    def send_totals(g):
        t_copies[g] = [
            send(tb.at[g, me], tb.at[g, me], t_send.at[g, k], t_recv.at[g, k],
                 {"sp": lax.rem(me + k, n)})
            for k in range(1, n)
        ]

    def send_near(h):
        y_copies[h] = []
        for k in range(1, near):
            y = lax.rem(my_near + k, near)
            y_copies[h].append(
                send(bs.at[h, y], ry.at[h, k - 1], y_send.at[h, k - 1], y_recv.at[h, k - 1],
                     {"sp": my_far * near + y})
            )

    def scale_after(h, block):
        total = jnp.ones((seqs, HD), F32)
        for b in range(n):
            total = total * jnp.where(b > block, tb[h // GROUP, b, h % GROUP], 1.0)
        return total

    def combine(h):
        sources = [lax.rem(my_near + near - k, near) for k in range(near)]
        scales = [scale_after(h, my_far * near + y) for y in sources]
        fill = HD - near * seqs
        cols = jnp.concatenate(scales + [jnp.zeros((fill, HD), F32)], axis=0).T
        for f in range(far):
            for y in range(near):
                lo = (f * near + y) * share
                lcol[h, y, f] = cols[lo : lo + share]
        for cp in y_copies[h]:
            cp.wait_recv()
        for f in range(far):
            col = lcol[h, my_near, f]
            for s in range(seqs):
                total = bs[h, my_near, f, s] * col[:, s : s + 1]
                for k in range(1, near):
                    j = k * seqs + s
                    total += ry[h, k - 1, f, s] * col[:, j : j + 1]
                pz[h, f, s] = total
        z_copies[h] = []
        for k in range(1, far):
            f = lax.rem(my_far + k, far)
            z_copies[h].append(
                send(pz.at[h, f], rz.at[h, k - 1], z_send.at[h, k - 1], z_recv.at[h, k - 1],
                     {"sp": f * near + my_near})
            )

    def finish(h):
        for cp in z_copies[h]:
            cp.wait_recv()
        for s in range(seqs):
            total = pz[h, my_far, s]
            for k in range(1, far):
                total += rz[h, k - 1, s]
            state_out[h, s] = total.astype(BF16)

    def token_terms(h, block):
        lo = h % GROUP * HD
        new_pre = block[0:seqs, lo : lo + HD].astype(BF16).astype(F32)
        new_value = block[0:seqs, wide + lo : wide + lo + HD].astype(BF16).astype(F32)
        new_key = (1.0 - lanes(lower, h)) / (1.0 + jnp.exp(new_pre))
        q = query[:, pl.ds(h * HD, HD)].astype(F32)
        q = q / (1.0 + jnp.exp(-q))
        qk[h] = q * (1.0 - new_key)
        kv[h] = jnp.sum(q * new_key, axis=1, keepdims=True) * new_value

    def read_part(h):
        row = qk[h] * scale_after(h, me)
        col = jnp.concatenate([row, jnp.zeros((HD - seqs, HD), F32)], axis=0).T
        for s in range(seqs):
            total = jnp.zeros((share, HD), F32)
            for f in range(far):
                for y in range(near):
                    lo = (f * near + y) * share
                    total += bs[h, y, f, s] * col[lo : lo + share, s : s + 1]
            rp[me, h, pl.ds(s, 1), :] = jnp.sum(total, axis=0, keepdims=True)

    def take_tokens():
        for cp in tok_copies:
            cp.wait_recv()
        xs[pl.ds(rows, PAD), :] = jnp.zeros((PAD, depth), BF16)
        for c in range(m):
            xs[pl.ds(rows, seqs), pl.ds(c * tk, tk)] = toks[c]

    def take_totals(g):
        for cp in t_copies[g]:
            cp.wait_recv()

    def members(g):
        return range(g * GROUP, (g + 1) * GROUP)

    for g in range(groups):
        if g == 1:
            take_tokens()
        matmul(g)
        if g == 0:
            e_copy.wait()
        for h in members(g):
            gate(h)
        send_totals(g)
        for h in members(g):
            send_near(h)
        if g >= 1:
            for h in members(g):
                token_terms(h, acc[g % 2, pl.ds(rows, PAD), :])
            take_totals(g - 1)
            for h in members(g - 1):
                combine(h)
        if g >= 2:
            for h in members(g - 2):
                finish(h)
    if groups == 1:
        take_tokens()
    first = jnp.dot(xs[pl.ds(rows, PAD), :], ws[0], preferred_element_type=F32)
    for h in members(0):
        token_terms(h, first)
    last = groups - 1
    for h in range(last * GROUP):
        read_part(h)
    take_totals(last)
    for h in members(last):
        read_part(h)
    r_copies = [
        send(rp.at[me], rp.at[me], r_send.at[k], r_recv.at[k], {"sp": lax.rem(me + k, n)})
        for k in range(1, n)
    ]
    for h in members(last):
        combine(h)
    if groups > 1:
        for h in members(last - 1):
            finish(h)
    for cp in r_copies:
        cp.wait_recv()
    for h in range(heads):
        raw = kv[h]
        for b in range(n):
            raw = raw + rp[b, h]
        mean = jnp.mean(raw * raw, axis=1, keepdims=True)
        normed = raw * lax.rsqrt(mean + 1e-6) * lanes(gain, 0)
        read_out[:, pl.ds(h * HD, HD)] = normed.astype(BF16)
    for h in members(last):
        finish(h)
    for cp in sends:
        cp.wait_send()


def local(n, m, prompt, forget_w, value_w, lower, extra, token, query, gain):
    seqs, span, depth = prompt.shape
    rows = seqs * span
    width = forget_w.shape[1]
    heads = width // HD
    groups = heads // GROUP
    share = HD // n
    near = near_size(n)
    far = n // near
    vmem = pl.BlockSpec(memory_space=pltpu.VMEM)
    hbm = pl.BlockSpec(memory_space=pl.ANY)
    dma = pltpu.SemaphoreType.DMA
    state, read = pl.pallas_call(
        functools.partial(kernel, n, m, near),
        out_shape=(
            jax.ShapeDtypeStruct((heads, seqs, share, HD), BF16),
            jax.ShapeDtypeStruct((seqs, width), BF16),
        ),
        in_specs=[hbm, hbm, hbm, vmem, hbm, vmem, vmem, vmem],
        out_specs=(vmem, vmem),
        scratch_shapes=[
            pltpu.VMEM((rows + PAD, depth), BF16),
            pltpu.VMEM((groups, depth, 2 * GROUP * HD), BF16),
            pltpu.VMEM((seqs, span, width), F32),
            pltpu.VMEM((2, rows + PAD, 2 * GROUP * HD), F32),
            pltpu.VMEM((m, seqs, token.shape[1]), BF16),
            pltpu.VMEM((heads, near, far, seqs, share, HD), F32),
            pltpu.VMEM((heads, near - 1, far, seqs, share, HD), F32),
            pltpu.VMEM((heads, far, seqs, share, HD), F32),
            pltpu.VMEM((heads, far - 1, seqs, share, HD), F32),
            pltpu.VMEM((groups, n, GROUP, seqs, HD), F32),
            pltpu.VMEM((n, heads, seqs, HD), F32),
            pltpu.VMEM((heads, near, far, share, HD), F32),
            pltpu.VMEM((heads, seqs, HD), F32),
            pltpu.VMEM((heads, seqs, HD), F32),
            dma((CHUNKS, seqs)),
            dma((groups, CHUNKS, 2)),
            dma,
            dma((m,)),
            dma((m,)),
            dma((groups, n)),
            dma((groups, n)),
            dma((heads, near - 1)),
            dma((heads, near - 1)),
            dma((heads, far - 1)),
            dma((heads, far - 1)),
            dma((n,)),
            dma((n,)),
        ],
        compiler_params=pltpu.CompilerParams(collective_id=0, has_side_effects=True),
    )(prompt, forget_w, value_w, lower, extra, token, query, gain)
    return state.transpose(2, 0, 1, 3), read


def solution(mesh):
    return jax.shard_map(
        functools.partial(local, mesh.shape["sp"], mesh.shape["tp"]),
        mesh=mesh,
        in_specs=(
            P(None, "sp", None),
            P(None, "tp"),
            P(None, "tp"),
            P("tp"),
            P(None, "sp", "tp"),
            P(None, "tp"),
            P(None, "tp"),
            P(),
        ),
        out_specs=(P("sp", "tp", None, None), P(None, "tp")),
        check_vma=False,
    )
```
